32 devices in a mesh: sp: 8 (over z, x), dp: 4 (over y, core).
Axes of the slice: x: 2, y: 2, z: 4, core: 2. Of those that a mesh axis runs over, the one named last changes fastest.
Arguments:
- residual_in: bfloat16 [4, 1024, 2048], P('dp', 'sp'), may hold values from -6 to 6
- query_proj: bfloat16 [4, 1024, 2048], P('dp', 'sp'), may hold values from -8 to 8
- key_proj: bfloat16 [4, 1024, 512], P('dp', 'sp'), may hold values from -8 to 8
- value_proj: bfloat16 [4, 1024, 512], P('dp', 'sp'), may hold values from -6 to 6
- query_gain: float32 [128], replicated, may hold values from 0.1 to 7
- key_gain: float32 [128], replicated, may hold values from 0.1 to 7
- out_weight: bfloat16 [2048, 2048], replicated, may hold values from -0.125 to 0.125
- post_gain: float32 [2048], replicated, may hold values from 0.1 to 1.9
- pre_gain: float32 [2048], replicated, may hold values from 0.1 to 1.9
- route_ids: int32 [4, 1024, 2], P('dp', 'sp'), may hold values from 0 to 31, as said below
- group_weight: float32 [4, 1024], P('dp', 'sp'), may hold values from 0.25 to 1
- first_share: float32 [4, 1024], P('dp', 'sp'), may hold values from 0.5 to 1
- gate_weight: bfloat16 [32, 2048, 512], P(('sp', 'dp')), may hold values from -0.125 to 0.125
- up_weight: bfloat16 [32, 2048, 512], P(('sp', 'dp')), may hold values from -0.125 to 0.125
- down_weight: bfloat16 [32, 512, 2048], P(('sp', 'dp')), may hold values from -0.25 to 0.25
Outputs:
- layer_out: bfloat16 [4, 1024, 2048], P('dp', 'sp')
The draws below stay inside these ranges and needn't reach their ends.
Inputs may be any that keep to these rules, and one draw needn't show every extreme that they name: `route_ids`: each token names two different experts of one group of 8 consecutive experts. Among the 128 tokens of one device each group is chosen by exactly 32 tokens, no expert is named by more than 16 of them, and in every draw one expert of each group is named by exactly 16 tokens of every device.
All inputs are finite; a program needn't handle non-finite values.
Results may differ from the reference program's by a relative error of at most 0.009.
The reference program's roundings to bfloat16 on the way count: a program that leaves them out, or rounds other values in their place, can miss the bound.
Values may be sent and summed in bfloat16 or wider, within the bound.
No kernel may reach another device: no remote copies, remote signals or barrier semaphores. Data moves between devices by JAX's collectives and lax.ppermute only.
A program may use at most 128 MiB of HBM per device.

```python
import jax
import jax.numpy as jnp
from jax import lax

D = 2048
HEADS = 16
KV_HEADS = 4
HEAD_DIM = 128
FF = 512
GROUPS = 4
GRID_W = 64
TOK_DEV = 128
SEQS = 4
SEQ = 1024
EXPERTS = 32
CAP = 16
N_SP = 8
N_DP = 4


def draw_query_proj(key, part):
    own = jax.random.fold_in(key, 11)
    base = jax.random.truncated_normal(own, -6.0, 6.0, (SEQS, SEQ, HEADS * HEAD_DIM), jnp.float32)
    return base.astype(jnp.bfloat16)


def draw_key_proj(key, part):
    own = jax.random.fold_in(key, 12)
    base = jax.random.truncated_normal(own, -6.0, 6.0, (SEQS, SEQ, KV_HEADS * HEAD_DIM), jnp.float32)
    return base.astype(jnp.bfloat16)


def gain_table(own):
    return 1.0 + 0.18 * jax.random.truncated_normal(own, -5.0, 5.0, (HEAD_DIM,), jnp.float32)


def draw_query_gain(key, part):
    return gain_table(jax.random.fold_in(key, 21))


def draw_key_gain(key, part):
    return gain_table(jax.random.fold_in(key, 22))


def draw_route_ids(key, part):
    per_group = TOK_DEV // GROUPS
    group_width = EXPERTS // GROUPS
    middle = CAP // 2
    hot = jax.random.randint(jax.random.fold_in(key, 31), (GROUPS,), 0, group_width)
    block_count = SEQS * (SEQ // TOK_DEV)

    def one_block(block_key):
        key_tok, key_rest = jax.random.split(block_key)
        order = jax.random.permutation(key_tok, TOK_DEV)
        firsts = []
        seconds = []
        for group_id in range(GROUPS):
            group_key = jax.random.fold_in(key_rest, group_id)
            key_perm, key_shift, key_swap = jax.random.split(group_key, 3)
            shuffled = jax.random.permutation(key_perm, group_width).astype(jnp.int32)
            shifts = jax.random.randint(key_shift, (group_width // 2,), -middle, middle + 1)
            hot_place = jnp.sum(jnp.where(shuffled == hot[group_id], jnp.arange(group_width, dtype=jnp.int32), 0))
            sign_value = 1 - 2 * (hot_place % 2)
            shifts = shifts.at[hot_place // 2].set(middle * sign_value)
            counts = jnp.zeros((group_width,), jnp.int32).at[shuffled[0::2]].set(middle + shifts).at[shuffled[1::2]].set(middle - shifts)
            listed = jnp.repeat(jnp.arange(group_width, dtype=jnp.int32), counts, total_repeat_length=2 * per_group)
            first_pick = listed[:per_group]
            second_pick = listed[per_group:]
            swap_bits = jax.random.randint(key_swap, (per_group,), 0, 2)
            leading = jnp.where(swap_bits == 1, second_pick, first_pick)
            trailing = jnp.where(swap_bits == 1, first_pick, second_pick)
            firsts.append(leading + group_id * group_width)
            seconds.append(trailing + group_id * group_width)
        pairs = jnp.stack([jnp.concatenate(firsts), jnp.concatenate(seconds)], axis=1).astype(jnp.int32)
        return jnp.zeros((TOK_DEV, 2), jnp.int32).at[order].set(pairs)
    blocks_all = jax.vmap(one_block)(jax.random.split(jax.random.fold_in(key, 32), block_count))
    return blocks_all.reshape(SEQS, SEQ, 2)


def level_of(rng, shape, cuts, least, top_value):
    level, own = 1.0, jax.random.fold_in(rng, 6)
    for axis_at, shards_of in cuts:
        steps = jnp.exp(jax.random.uniform(jax.random.fold_in(own, axis_at), (shards_of,), jnp.float32, least / len(cuts), top_value / len(cuts)))
        level = level * jnp.repeat(steps, shape[axis_at] // shards_of).reshape([-1 if axis == axis_at else 1 for axis in range(len(shape))])
    return level


def bell_draw(key, shape, deviation, bound, cuts=(), kind=jnp.bfloat16):
    entries = jax.random.normal(key, shape, jnp.float32) * deviation
    if len(cuts) > 0:
        entries = level_of(key, shape, cuts, -0.22, 0.18) * entries
    return jnp.clip(entries, min=-bound, max=bound).astype(kind)


def setup_inputs(seed: int = 0) -> dict:
    keys = jax.random.split(jax.random.key(seed), 16)
    residual_in = bell_draw(keys[0], (SEQS, SEQ, D), 1.0, 6.0, ((0, 4), (1, 8)))
    query_proj = draw_query_proj(jax.random.fold_in(keys[15], 71), 0)
    key_proj = draw_key_proj(jax.random.fold_in(keys[15], 71), 0)
    value_proj = bell_draw(keys[3], (SEQS, SEQ, KV_HEADS * HEAD_DIM), 1.0, 6.0, ((0, 4), (1, 8)))
    query_gain = draw_query_gain(jax.random.fold_in(keys[15], 71), 0)
    key_gain = draw_key_gain(jax.random.fold_in(keys[15], 71), 0)
    out_weight = bell_draw(keys[6], (D, D), D ** -0.5, 0.125)
    post_gain = jnp.clip(1.0 + 0.18 * jax.random.normal(keys[7], (D,), jnp.float32), 0.1, 1.9)
    pre_gain = jnp.clip(1.0 + 0.18 * jax.random.normal(keys[8], (D,), jnp.float32), 0.1, 1.9)
    route_ids = draw_route_ids(jax.random.fold_in(keys[15], 71), 0)
    group_weight = jnp.clip(0.25 + 0.75 * jax.random.uniform(keys[10], (SEQS, SEQ), jnp.float32) ** level_of(keys[10], (SEQS, SEQ), ((0, 4), (1, 8)), -0.2, 0.2), 0.25, 1.0)
    first_share = jnp.clip(0.5 + 0.5 * jax.random.uniform(keys[11], (SEQS, SEQ), jnp.float32) ** level_of(keys[11], (SEQS, SEQ), ((0, 4), (1, 8)), -0.2, 0.2), 0.5, 1.0)
    gate_weight = bell_draw(keys[12], (EXPERTS, D, FF), D ** -0.5, 0.125, ((0, 32),))
    up_weight = bell_draw(keys[13], (EXPERTS, D, FF), D ** -0.5, 0.125, ((0, 32),))
    down_weight = bell_draw(keys[14], (EXPERTS, FF, D), FF ** -0.5, 0.25, ((0, 32),))
    return {"residual_in": residual_in, "query_proj": query_proj, "key_proj": key_proj, "value_proj": value_proj, "query_gain": query_gain, "key_gain": key_gain, "out_weight": out_weight, "post_gain": post_gain, "pre_gain": pre_gain, "route_ids": route_ids, "group_weight": group_weight, "first_share": first_share, "gate_weight": gate_weight, "up_weight": up_weight, "down_weight": down_weight}


EPSILON = 1e-06

def rotate_heads(raw_heads, gain_vec, positions):
    floats = raw_heads.astype(jnp.float32)
    normed = floats * lax.rsqrt(lax.optimization_barrier(jnp.mean(floats * floats, axis=-1, keepdims=True)) + EPSILON) * gain_vec
    quarter = raw_heads.shape[-1] // 4
    inverse = 10000.0 ** (-jnp.arange(quarter, dtype=jnp.float32) / quarter)
    grid_rows = (positions // GRID_W).astype(jnp.float32)[:, None] * inverse
    grid_cols = (positions % GRID_W).astype(jnp.float32)[:, None] * inverse
    angles = jnp.concatenate([grid_rows, grid_rows, grid_cols, grid_cols], axis=-1)[:, None, :]
    pieces = normed.reshape(normed.shape[:-1] + (2, 2, quarter))
    turned = jnp.stack([-pieces[..., 1, :], pieces[..., 0, :]], axis=-2).reshape(normed.shape)
    return (normed * jnp.cos(angles) + turned * jnp.sin(angles)).astype(jnp.bfloat16)

def attend_blocks(queries, keys_all, values_all):
    count_q, kv_count, group_size, head_width = queries.shape
    block = min(512, count_q)
    blocks = count_q // block
    scale = head_width ** (-0.5)
    zero_index = jnp.zeros((), jnp.int32)

    def one_item(item):
        which = (item // kv_count).astype(jnp.int32)
        head_index = (item % kv_count).astype(jnp.int32)
        start_row = (which * block).astype(jnp.int32)
        q_block = lax.dynamic_slice(queries, (start_row, head_index, zero_index, zero_index), (block, 1, group_size, head_width))[:, 0]
        key_block = lax.dynamic_slice(keys_all, (zero_index, head_index, zero_index), (keys_all.shape[0], 1, head_width))[:, 0]
        value_block = lax.dynamic_slice(values_all, (zero_index, head_index, zero_index), (values_all.shape[0], 1, head_width))[:, 0]
        scores = jnp.einsum('qgd,sd->gqs', q_block.astype(jnp.float32), key_block.astype(jnp.float32)) * scale
        shifted = jnp.exp(scores - lax.optimization_barrier(jnp.max(scores, axis=-1, keepdims=True)))
        weights = (shifted / lax.optimization_barrier(jnp.sum(shifted, axis=-1, keepdims=True))).astype(jnp.bfloat16)
        return jnp.einsum('gqs,sd->qgd', weights.astype(jnp.float32), value_block.astype(jnp.float32)).astype(jnp.bfloat16)
    results = lax.map(one_item, jnp.arange(blocks * kv_count, dtype=jnp.int32))
    results = results.reshape(blocks, kv_count, block, group_size, head_width).transpose(0, 2, 1, 3, 4)
    return results.reshape(count_q, kv_count * group_size * head_width)

def rms_scale(values, gain_vec):
    floats = values.astype(jnp.float32)
    return floats * lax.rsqrt(lax.optimization_barrier(jnp.mean(floats * floats, axis=-1, keepdims=True)) + EPSILON) * gain_vec

def reference(residual_in, query_proj, key_proj, value_proj, query_gain, key_gain, out_weight, post_gain, pre_gain, route_ids, group_weight, first_share, gate_weight, up_weight, down_weight):
    group_size = HEADS // KV_HEADS

    def one_sequence(inputs):
        query_seq, key_seq, value_seq = inputs
        positions = jnp.arange(SEQ, dtype=jnp.int32)
        query_turned = rotate_heads(query_seq.reshape(SEQ, HEADS, HEAD_DIM), query_gain, positions)
        key_turned = rotate_heads(key_seq.reshape(SEQ, KV_HEADS, HEAD_DIM), key_gain, positions)
        return attend_blocks(query_turned.reshape(SEQ, KV_HEADS, group_size, HEAD_DIM), key_turned, value_seq.reshape(SEQ, KV_HEADS, HEAD_DIM))
    attended = lax.map(one_sequence, (query_proj, key_proj, value_proj)).reshape(SEQS * SEQ, D)
    mixed = jnp.dot(attended, out_weight, preferred_element_type=jnp.float32).astype(jnp.bfloat16)
    stream = (residual_in.reshape(SEQS * SEQ, D).astype(jnp.float32) + rms_scale(mixed, post_gain)).astype(jnp.bfloat16)
    normed = rms_scale(stream, pre_gain).astype(jnp.bfloat16)
    chosen = route_ids.reshape(-1).astype(jnp.int32)
    assigns = chosen.shape[0]
    order = jnp.argsort(chosen, stable=True).astype(jnp.int32)
    counts = jax.ops.segment_sum(jnp.ones((assigns,), jnp.int32), chosen, num_segments=EXPERTS).astype(jnp.int32)
    starts = (jnp.cumsum(counts) - counts).astype(jnp.int32)
    most = CAP * N_SP * N_DP
    order_pad = jnp.concatenate([order, jnp.full((most,), assigns, jnp.int32)])
    normed_pad = jnp.concatenate([normed, jnp.zeros((1, D), jnp.bfloat16)], axis=0)

    def per_expert(carry, inputs):
        index, gate_one, up_one, down_one = inputs
        picked = lax.dynamic_slice(order_pad, (starts[index].astype(jnp.int32),), (most,))
        valid = jnp.arange(most, dtype=jnp.int32) < counts[index]
        picked = jnp.where(valid, picked, assigns).astype(jnp.int32)
        rows_in = normed_pad[picked // 2]
        gated = jnp.dot(rows_in, gate_one, preferred_element_type=jnp.float32)
        lifted = jnp.dot(rows_in, up_one, preferred_element_type=jnp.float32)
        hidden = (jax.nn.silu(gated) * lifted).astype(jnp.bfloat16)
        produced = jnp.dot(hidden, down_one, preferred_element_type=jnp.float32).astype(jnp.bfloat16)
        return (carry.at[picked].set(produced), None)
    outputs, _ = lax.scan(per_expert, jnp.zeros((assigns + 1, D), jnp.bfloat16), (jnp.arange(EXPERTS, dtype=jnp.int32), gate_weight, up_weight, down_weight))
    results = outputs[:assigns].astype(jnp.float32).reshape(SEQS * SEQ, 2, D)
    share = first_share.reshape(-1)
    weight_pair = group_weight.reshape(-1)[:, None] * jnp.stack([share, 1.0 - share], axis=1)
    combined = lax.optimization_barrier(jnp.sum(weight_pair[:, :, None] * results, axis=1))
    return (stream.astype(jnp.float32) + combined).astype(jnp.bfloat16).reshape(SEQS, SEQ, D)
```

```python
import functools
import itertools

import jax
import jax.numpy as jnp
from jax import lax
from jax.experimental import pallas as pl
from jax.experimental.pallas import tpu as pltpu
from jax.sharding import Mesh
from jax.sharding import PartitionSpec as P

HEADS = 16
KV_HEADS = 4
HEAD_DIM = 128
GRID_W = 64
GROUPS = 4
CORES = 2
LANES = 128


EPSILON = 1e-06


def rotate_heads(raw_heads, gain_vec, positions):
    floats = raw_heads.astype(jnp.float32)
    normed = (
        floats * lax.rsqrt(jnp.mean(floats * floats, axis=-1, keepdims=True) + EPSILON) * gain_vec
    )
    quarter = raw_heads.shape[-1] // 4
    inverse = 10000.0 ** (-jnp.arange(quarter, dtype=jnp.float32) / quarter)
    grid_rows = (positions // GRID_W).astype(jnp.float32)[:, None] * inverse
    grid_cols = (positions % GRID_W).astype(jnp.float32)[:, None] * inverse
    angles = jnp.concatenate([grid_rows, grid_rows, grid_cols, grid_cols], axis=-1)[:, None, :]
    pieces = normed.reshape(normed.shape[:-1] + (2, 2, quarter))
    turned = jnp.stack([-pieces[..., 1, :], pieces[..., 0, :]], axis=-2).reshape(normed.shape)
    return (normed * jnp.cos(angles) + turned * jnp.sin(angles)).astype(jnp.bfloat16)


def attend_blocks(queries, keys_all, values_all):
    count_q, kv_count, group_size, head_width = queries.shape
    block = min(512, count_q)
    blocks = count_q // block
    scale = head_width ** (-0.5)
    zero_index = jnp.zeros((), jnp.int32)

    def one_item(item):
        which = item // kv_count
        head_index = item % kv_count
        start_row = which * block
        q_block = lax.dynamic_slice(
            queries,
            (start_row, head_index, zero_index, zero_index),
            (block, 1, group_size, head_width),
        )[:, 0]
        key_block = lax.dynamic_slice(
            keys_all, (zero_index, head_index, zero_index), (keys_all.shape[0], 1, head_width)
        )[:, 0]
        value_block = lax.dynamic_slice(
            values_all, (zero_index, head_index, zero_index), (values_all.shape[0], 1, head_width)
        )[:, 0]
        scores = (
            jnp.einsum("qgd,sd->gqs", q_block, key_block, preferred_element_type=jnp.float32)
            * scale
        )
        shifted = jnp.exp(scores - jnp.max(scores, axis=-1, keepdims=True))
        weights = (shifted / jnp.sum(shifted, axis=-1, keepdims=True)).astype(jnp.bfloat16)
        return jnp.einsum(
            "gqs,sd->qgd", weights, value_block, preferred_element_type=jnp.float32
        ).astype(jnp.bfloat16)

    results = lax.map(one_item, jnp.arange(blocks * kv_count, dtype=jnp.int32))
    results = results.reshape(blocks, kv_count, block, group_size, head_width).transpose(
        0, 2, 1, 3, 4
    )
    return results.reshape(count_q, kv_count * group_size * head_width)


def rms_scale(values, gain_vec):
    floats = values.astype(jnp.float32)
    return (
        floats * lax.rsqrt(jnp.mean(floats * floats, axis=-1, keepdims=True) + EPSILON) * gain_vec
    )


def expert_ffn(arrived, gate_weight, up_weight, down_weight):
    gated = jnp.einsum("nesd,edf->nesf", arrived, gate_weight, preferred_element_type=jnp.float32)
    lifted = jnp.einsum("nesd,edf->nesf", arrived, up_weight, preferred_element_type=jnp.float32)
    hidden = (jax.nn.silu(gated) * lifted).astype(jnp.bfloat16)
    return jnp.einsum(
        "nesf,efd->nesd", hidden, down_weight, preferred_element_type=jnp.float32
    ).astype(jnp.bfloat16)


def local_any(
    residual_in,
    query_proj,
    key_proj,
    value_proj,
    query_gain,
    key_gain,
    out_weight,
    post_gain,
    pre_gain,
    route_ids,
    group_weight,
    first_share,
    gate_weight,
    up_weight,
    down_weight,
):
    sp_count = lax.axis_size("sp")
    dp_count = lax.axis_size("dp")
    tokens = query_proj.shape[1]
    group_size = HEADS // KV_HEADS
    key_all, value_all = (
        lax.all_gather(key_proj, "sp", axis=1, tiled=True),
        lax.all_gather(value_proj, "sp", axis=1, tiled=True),
    )
    length = key_all.shape[1]
    key_positions = jnp.arange(length, dtype=jnp.int32)
    query_positions = lax.axis_index("sp") * tokens + jnp.arange(tokens, dtype=jnp.int32)
    query_turned = rotate_heads(
        query_proj.reshape(tokens, HEADS, HEAD_DIM), query_gain, query_positions
    )
    key_turned = rotate_heads(key_all.reshape(length, KV_HEADS, HEAD_DIM), key_gain, key_positions)
    attended = attend_blocks(
        query_turned.reshape(tokens, KV_HEADS, group_size, HEAD_DIM),
        key_turned,
        value_all.reshape(length, KV_HEADS, HEAD_DIM),
    )
    mixed = jnp.dot(attended, out_weight, preferred_element_type=jnp.float32).astype(jnp.bfloat16)
    stream = (residual_in[0].astype(jnp.float32) + rms_scale(mixed, post_gain)).astype(jnp.bfloat16)
    normed = rms_scale(stream, pre_gain).astype(jnp.bfloat16)
    model_width = normed.shape[1]
    local_experts = gate_weight.shape[0]
    expert_count = local_experts * sp_count * dp_count
    capacity = 4 * tokens // expert_count
    chosen = route_ids.reshape(2 * tokens)
    onehot = (chosen[:, None] == jnp.arange(expert_count, dtype=jnp.int32)[None, :]).astype(
        jnp.int32
    )
    earlier = jnp.cumsum(onehot, axis=0) - onehot
    slot_rank = jnp.sum(earlier * onehot, axis=1)
    slot_index = chosen * capacity + slot_rank
    source_row = (
        jnp.full((expert_count * capacity,), tokens, jnp.int32)
        .at[slot_index]
        .set(jnp.arange(2 * tokens, dtype=jnp.int32) // 2)
    )
    padded = jnp.concatenate([normed, jnp.zeros((1, model_width), jnp.bfloat16)], axis=0)
    outgoing = padded[source_row]
    shaped = outgoing.reshape(sp_count * dp_count, local_experts, capacity, model_width)
    answered = expert_ffn(
        lax.all_to_all(shaped, ("sp", "dp"), split_axis=0, concat_axis=0, tiled=True),
        gate_weight,
        up_weight,
        down_weight,
    )
    returned = lax.all_to_all(answered, ("sp", "dp"), split_axis=0, concat_axis=0, tiled=True)
    results = (
        returned.reshape(expert_count * capacity, model_width)[slot_index]
        .astype(jnp.float32)
        .reshape(tokens, 2, model_width)
    )
    share = first_share[0]
    weight_pair = group_weight[0][:, None] * jnp.stack([share, 1.0 - share], axis=1)
    combined = jnp.sum(weight_pair[:, :, None] * results, axis=1)
    return (
        (stream.astype(jnp.float32) + combined).astype(jnp.bfloat16).reshape(1, tokens, model_width)
    )


def solution_any(mesh):
    placed = (
        P("dp", "sp", None),
        P("dp", "sp", None),
        P("dp", "sp", None),
        P("dp", "sp", None),
        P(),
        P(),
        P(),
        P(),
        P(),
        P("dp", "sp", None),
        P("dp", "sp"),
        P("dp", "sp"),
        P(("sp", "dp"), None, None),
        P(("sp", "dp"), None, None),
        P(("sp", "dp"), None, None),
    )
    return jax.shard_map(
        local_any, mesh=mesh, in_specs=placed, out_specs=P("dp", "sp", None), check_vma=False
    )


def turn(floats, gain, cos, sin):
    normed = floats * lax.rsqrt(jnp.mean(floats * floats, axis=-1, keepdims=True) + EPSILON) * gain
    quarter = floats.shape[-1] // 4
    lane = lax.broadcasted_iota(jnp.int32, floats.shape, 1)
    ahead = pltpu.roll(normed, floats.shape[-1] - quarter, 1)
    behind = pltpu.roll(normed, quarter, 1)
    turned = jnp.where((lane // quarter) % 2 == 0, ahead, behind)
    return (normed * cos + turned * sin).astype(jnp.bfloat16)


def mid_kernel(
    blocks,
    chunks,
    block_ids,
    query,
    residual,
    meta,
    row_table,
    col_table,
    query_gain,
    key_gain,
    post_gain,
    pre_gain,
    weight_hbm,
    *rest,
):
    kv = rest[:blocks]
    stream_out = rest[blocks]
    row_outs = rest[blocks + 1 : blocks + 1 + chunks]
    weight, keys, values, turned, attended, mixed, payload, semaphore = rest[blocks + 1 + chunks :]
    copy = pltpu.make_async_copy(weight_hbm, weight, semaphore)
    copy.start()
    tokens, width = query.shape
    lines = tokens // GRID_W
    key_width = KV_HEADS * HEAD_DIM
    group = HEADS // KV_HEADS
    key_scale = key_gain[...]
    query_scale = query_gain[...]

    def table(block, line):
        row = pl.ds(block_ids[block] * lines + line, 1)
        cos = row_table[0, row, :] + col_table[0]
        sin = row_table[1, row, :] + col_table[1]
        return cos, sin

    for block in range(blocks):
        base = block * tokens
        values[base : base + tokens, :] = kv[block][:, key_width:]
        for line in range(lines):
            cos, sin = table(block, line)
            here = slice(line * GRID_W, (line + 1) * GRID_W)
            for head in range(KV_HEADS):
                columns = slice(head * HEAD_DIM, (head + 1) * HEAD_DIM)
                raw = kv[block][here, columns].astype(jnp.float32)
                keys[base + line * GRID_W : base + (line + 1) * GRID_W, columns] = turn(
                    raw, key_scale, cos, sin
                )

    for line in range(lines):
        cos, sin = table(blocks, line)
        here = slice(line * GRID_W, (line + 1) * GRID_W)
        for head in range(HEADS):
            columns = slice(head * HEAD_DIM, (head + 1) * HEAD_DIM)
            raw = query[here, columns].astype(jnp.float32)
            start = (head % group) * tokens + line * GRID_W
            turned[head // group, start : start + GRID_W, :] = turn(raw, query_scale, cos, sin)

    factor = HEAD_DIM**-0.5 * 1.4426950408889634

    @pl.loop(0, KV_HEADS)
    def _(head):
        columns = pl.ds(pl.multiple_of(head * HEAD_DIM, HEAD_DIM), HEAD_DIM)
        scores = lax.dot_general(
            turned[head],
            keys[:, columns],
            (((1,), (1,)), ((), ())),
            preferred_element_type=jnp.float32,
        )
        top = jnp.max(scores, axis=-1, keepdims=True)
        shifted = jnp.exp2((scores - top) * factor)
        total = jnp.sum(shifted, axis=-1, keepdims=True)
        probs = (shifted * (1.0 / total)).astype(jnp.bfloat16)
        result = jnp.dot(probs, values[:, columns], preferred_element_type=jnp.float32)
        for part in range(group):
            target = pl.ds(
                pl.multiple_of((head * group + part) * HEAD_DIM, HEAD_DIM), HEAD_DIM
            )
            attended[:, target] = result[part * tokens : (part + 1) * tokens].astype(jnp.bfloat16)

    copy.wait()
    step = 4 * HEAD_DIM

    @pl.loop(0, width // step)
    def _(index):
        columns = pl.ds(pl.multiple_of(index * step, step), step)
        mixed[:, columns] = jnp.dot(
            attended[...], weight[:, columns], preferred_element_type=jnp.float32
        ).astype(jnp.bfloat16)

    raw = mixed[...].astype(jnp.float32)
    scaled = (
        raw * lax.rsqrt(jnp.mean(raw * raw, axis=-1, keepdims=True) + EPSILON) * post_gain[...]
    )
    stream = (residual[...].astype(jnp.float32) + scaled).astype(jnp.bfloat16)
    stream_out[...] = stream
    floats = stream.astype(jnp.float32)
    payload[:, :width] = (
        floats
        * lax.rsqrt(jnp.mean(floats * floats, axis=-1, keepdims=True) + EPSILON)
        * pre_gain[...]
    ).astype(jnp.bfloat16)
    payload[:, width:] = meta[...]
    slot = meta[:, LANES - 1 :].astype(jnp.float32)
    place = lax.broadcasted_iota(jnp.int32, (tokens, tokens), 1).astype(jnp.float32)
    choose = (slot == place).astype(jnp.bfloat16)
    ordered = lax.dot_general(
        choose, payload[...], (((0,), (0,)), ((), ())), preferred_element_type=jnp.float32
    ).astype(jnp.bfloat16)
    rows = tokens // chunks
    for chunk in range(chunks):
        row_outs[chunk][...] = ordered[chunk * rows : (chunk + 1) * rows]


def expert_kernel(count, merge, which, gate, up, down, *rest):
    inputs = rest[:count]
    outputs = rest[count:]
    width = gate.shape[0]
    block = jnp.concatenate([ref[:, :width] for ref in inputs], axis=0)
    meta = jnp.concatenate([ref[:, width:] for ref in inputs], axis=0).astype(jnp.float32)
    lane = lax.broadcasted_iota(jnp.int32, meta.shape, 1)
    mine = (lane == which[0]) | (lane == which[0] + LANES // 2)
    share = jnp.sum(jnp.where(mine, meta, 0.0), axis=-1, keepdims=True)
    gated = jnp.dot(block, gate[...], preferred_element_type=jnp.float32)
    lifted = jnp.dot(block, up[...], preferred_element_type=jnp.float32)
    hidden = (gated / (1.0 + jnp.exp(-gated)) * lifted).astype(jnp.bfloat16)
    produced = jnp.dot(hidden, down[...], preferred_element_type=jnp.float32).astype(jnp.bfloat16)
    weighted = (produced.astype(jnp.float32) * share).astype(jnp.bfloat16)
    base = 0
    for ref in outputs:
        ref[...] = weighted[base : base + ref.shape[0]]
        base += ref.shape[0]


def last_kernel(chunks, stream, meta, *rest):
    returned = rest[:chunks]
    out = rest[chunks]
    tokens = stream.shape[0]
    slot = meta[:, LANES - 1 :].astype(jnp.float32)
    place = lax.broadcasted_iota(jnp.int32, (tokens, tokens), 1).astype(jnp.float32)
    choose = (slot == place).astype(jnp.bfloat16)
    block = jnp.concatenate([ref[...] for ref in returned], axis=0)
    added = jnp.dot(choose, block, preferred_element_type=jnp.float32)
    out[...] = (stream[...].astype(jnp.float32) + added).astype(jnp.bfloat16)


VMEM = pl.BlockSpec(memory_space=pltpu.VMEM)
SMEM = pl.BlockSpec(memory_space=pltpu.SMEM)
ANY = pl.BlockSpec(memory_space=pl.ANY)


def shape_of(*dims):
    return jax.ShapeDtypeStruct(dims, jnp.bfloat16)


def local_plane(
    residual_in,
    query_proj,
    key_proj,
    value_proj,
    query_gain,
    key_gain,
    out_weight,
    post_gain,
    pre_gain,
    route_ids,
    group_weight,
    first_share,
    gate_weight,
    up_weight,
    down_weight,
):
    planes = lax.axis_size("z")
    xs, ys, cores = lax.axis_size("x"), lax.axis_size("y"), lax.axis_size("c")
    z, x, y, c = (lax.axis_index(name) for name in ("z", "x", "y", "c"))
    tokens, width = query_proj.shape[1:]
    rows = tokens // planes
    members = xs * ys * cores
    blocks = planes * cores

    def carry(value, jump):
        flat = lambda a, b, d: (a * xs + b) * cores + d
        route = [
            (flat(a, b, d), flat((a + jump) % planes, d, b))
            for a, b, d in itertools.product(range(planes), range(xs), range(cores))
        ]
        return lax.ppermute(value, ("z", "x", "c"), route)

    def shift(value, jump):
        return lax.ppermute(value, "z", [(a, (a + jump) % planes) for a in range(planes)])

    def swap(value, axis):
        return lax.ppermute(value, axis, [(0, 1), (1, 0)])

    kv = jnp.concatenate([key_proj[0], value_proj[0]], axis=1)
    kv_here = [carry(kv, jump) for jump in range(planes)]
    kv_there = [swap(block, "c") for block in kv_here]
    query = carry(query_proj[0], 0)
    residual = carry(residual_in[0], 0)

    ids = route_ids[0]
    group = ids[:, 0] // members
    jump_of = (group - z) % planes
    onehot = (group[:, None] == jnp.arange(planes, dtype=jnp.int32)).astype(jnp.float32)
    earlier = jnp.tril(jnp.ones((tokens, tokens), jnp.float32), -1)
    rank = jnp.sum(jnp.dot(earlier, onehot) * onehot, axis=1)
    slot = jump_of.astype(jnp.float32) * rows + rank
    share = first_share[0]
    pair = group_weight[0][:, None] * jnp.stack([share, 1.0 - share], axis=1)
    half = LANES // 2
    lane = jnp.arange(LANES, dtype=jnp.int32)
    spread = jnp.where((ids[:, :1] % members) == lane % half, pair[:, :1], 0.0) + jnp.where(
        (ids[:, 1:] % members) == lane % half, pair[:, 1:], 0.0
    )
    coarse = lax.reduce_precision(spread, 8, 7)
    meta = jnp.where(lane < half, coarse, spread - coarse)
    meta = jnp.where(lane == LANES - 1, slot[:, None], meta).astype(jnp.bfloat16)
    meta_here = carry(meta, 0)

    order = [(z - jump) % planes for jump in range(planes)]
    block_ids = jnp.stack(
        [a * cores + c for a in order] + [a * cores + (1 - c) for a in order] + [z * cores + c]
    ).astype(jnp.int32)
    quarter = HEAD_DIM // 4
    inverse = 10000.0 ** (-jnp.arange(quarter, dtype=jnp.float32) / quarter)
    lines = blocks * tokens // GRID_W

    def turns(count, columns):
        angles = jnp.arange(count, dtype=jnp.float32)[:, None] * inverse
        zeros = jnp.zeros((count, 2 * quarter), jnp.float32)
        cos = [jnp.cos(angles)] * 2
        sin = [-jnp.sin(angles), jnp.sin(angles)]
        if columns:
            return jnp.stack(
                [jnp.concatenate([zeros] + cos, 1), jnp.concatenate([zeros] + sin, 1)]
            )
        return jnp.stack([jnp.concatenate(cos + [zeros], 1), jnp.concatenate(sin + [zeros], 1)])

    payload = width + LANES
    key_width = KV_HEADS * HEAD_DIM
    length = blocks * tokens
    made = pl.pallas_call(
        functools.partial(mid_kernel, blocks, planes),
        out_shape=[shape_of(tokens, width)] + [shape_of(rows, payload)] * planes,
        in_specs=[SMEM] + [VMEM] * 9 + [ANY] + [VMEM] * blocks,
        out_specs=[VMEM] * (1 + planes),
        scratch_shapes=[
            pltpu.VMEM(out_weight.shape, jnp.bfloat16),
            pltpu.VMEM((length, key_width), jnp.bfloat16),
            pltpu.VMEM((length, key_width), jnp.bfloat16),
            pltpu.VMEM((KV_HEADS, tokens * HEADS // KV_HEADS, HEAD_DIM), jnp.bfloat16),
            pltpu.VMEM((tokens, width), jnp.bfloat16),
            pltpu.VMEM((tokens, width), jnp.bfloat16),
            pltpu.VMEM((tokens, payload), jnp.bfloat16),
            pltpu.SemaphoreType.DMA,
        ],
        cost_estimate=pl.CostEstimate(
            flops=2 * tokens * width * (2 * length + width),
            bytes_accessed=2 * width * width,
            transcendentals=tokens * HEADS * length,
        ),
        name="mid",
    )(
        block_ids,
        query,
        residual,
        meta_here,
        turns(lines, False),
        turns(GRID_W, True),
        query_gain[None],
        key_gain[None],
        post_gain[None],
        pre_gain[None],
        out_weight,
        *kv_here,
        *kv_there,
    )
    stream_here, sorted_rows = made[0], made[1:]
    own = jnp.concatenate([carry(value, jump) for jump, value in enumerate(sorted_rows)], axis=0)
    stream = carry(stream_here, 0)

    middle = tokens // 2
    by_x, by_y = swap(own, "x"), swap(own, "y")
    far = [swap(by_y[:middle], "x"), swap(by_x[middle:], "y")]
    which = ((x * ys + y) * cores + c).reshape(1).astype(jnp.int32)

    def experts(*pieces):
        inputs = list(pieces) + [swap(piece, "c") for piece in pieces]
        count = len(inputs)
        total = sum(piece.shape[0] for piece in inputs)
        return pl.pallas_call(
            functools.partial(expert_kernel, count, None),
            out_shape=[shape_of(tokens, width)] * cores,
            in_specs=[SMEM] + [VMEM] * (3 + count),
            out_specs=[VMEM] * cores,
            cost_estimate=pl.CostEstimate(
                flops=6 * total * width * gate_weight.shape[2],
                bytes_accessed=6 * width * gate_weight.shape[2],
                transcendentals=total * gate_weight.shape[2],
            ),
            name="experts",
        )(which, gate_weight[0], up_weight[0], down_weight[0], *inputs)

    def both(kept, sent):
        return kept + swap(sent, "c")

    sum_own = both(*experts(own))
    sum_x = both(*experts(by_x))
    sum_y = both(*experts(by_y))
    sum_far = both(*experts(*far))
    low_y = sum_y[:middle] + swap(sum_far[:middle], "x")
    high_x = sum_x[middle:] + swap(sum_far[middle:], "y")
    top = sum_own[:middle] + swap(sum_x[:middle], "x") + swap(low_y, "y")
    bottom = sum_own[middle:] + swap(high_x, "x") + swap(sum_y[middle:], "y")
    summed = jnp.concatenate([top, bottom], axis=0)
    returned = [
        shift(summed[jump * rows : (jump + 1) * rows], -jump) if jump else summed[:rows]
        for jump in range(planes)
    ]
    result = pl.pallas_call(
        functools.partial(last_kernel, planes),
        out_shape=shape_of(tokens, width),
        in_specs=[VMEM] * (2 + planes),
        out_specs=VMEM,
        cost_estimate=pl.CostEstimate(
            flops=2 * tokens * tokens * width, bytes_accessed=6 * tokens * width, transcendentals=0
        ),
        name="last",
    )(stream, meta, *returned)
    return result[None]


def solution(mesh):
    sp_count, dp_count = mesh.shape["sp"], mesh.shape["dp"]
    xs, ys = sp_count // GROUPS, dp_count // CORES
    if (xs, ys) != (2, 2) or xs != CORES:
        return solution_any(mesh)
    fine = Mesh(mesh.devices.reshape(GROUPS, xs, ys, CORES), ("z", "x", "y", "c"))
    tokens = P(("y", "c"), ("z", "x"), None)
    scalars = P(("y", "c"), ("z", "x"))
    experts = P(("z", "x", "y", "c"), None, None)
    placed = (tokens,) * 4 + (P(),) * 5 + (tokens, scalars, scalars) + (experts,) * 3
    return jax.shard_map(
        local_plane, mesh=fine, in_specs=placed, out_specs=tokens, check_vma=False
    )
```

```python
import functools
import itertools

import jax
import jax.numpy as jnp
from jax import lax
from jax.experimental import pallas as pl
from jax.experimental.pallas import tpu as pltpu
from jax.sharding import Mesh
from jax.sharding import PartitionSpec as P


HEADS = 16
KV_HEADS = 4
HEAD_DIM = 128
GRID_W = 64
GROUPS = 4
CORES = 2
LANES = 128


EPSILON = 1e-06


def rotate_heads(raw_heads, gain_vec, positions):
    floats = raw_heads.astype(jnp.float32)
    normed = (
        floats * lax.rsqrt(jnp.mean(floats * floats, axis=-1, keepdims=True) + EPSILON) * gain_vec
    )
    quarter = raw_heads.shape[-1] // 4
    inverse = 10000.0 ** (-jnp.arange(quarter, dtype=jnp.float32) / quarter)
    grid_rows = (positions // GRID_W).astype(jnp.float32)[:, None] * inverse
    grid_cols = (positions % GRID_W).astype(jnp.float32)[:, None] * inverse
    angles = jnp.concatenate([grid_rows, grid_rows, grid_cols, grid_cols], axis=-1)[:, None, :]
    pieces = normed.reshape(normed.shape[:-1] + (2, 2, quarter))
    turned = jnp.stack([-pieces[..., 1, :], pieces[..., 0, :]], axis=-2).reshape(normed.shape)
    return (normed * jnp.cos(angles) + turned * jnp.sin(angles)).astype(jnp.bfloat16)


def attend_blocks(queries, keys_all, values_all):
    count_q, kv_count, group_size, head_width = queries.shape
    block = min(512, count_q)
    blocks = count_q // block
    scale = head_width ** (-0.5)
    zero_index = jnp.zeros((), jnp.int32)

    def one_item(item):
        which = item // kv_count
        head_index = item % kv_count
        start_row = which * block
        q_block = lax.dynamic_slice(
            queries,
            (start_row, head_index, zero_index, zero_index),
            (block, 1, group_size, head_width),
        )[:, 0]
        key_block = lax.dynamic_slice(
            keys_all, (zero_index, head_index, zero_index), (keys_all.shape[0], 1, head_width)
        )[:, 0]
        value_block = lax.dynamic_slice(
            values_all, (zero_index, head_index, zero_index), (values_all.shape[0], 1, head_width)
        )[:, 0]
        scores = (
            jnp.einsum("qgd,sd->gqs", q_block, key_block, preferred_element_type=jnp.float32)
            * scale
        )
        shifted = jnp.exp(scores - jnp.max(scores, axis=-1, keepdims=True))
        weights = (shifted / jnp.sum(shifted, axis=-1, keepdims=True)).astype(jnp.bfloat16)
        return jnp.einsum(
            "gqs,sd->qgd", weights, value_block, preferred_element_type=jnp.float32
        ).astype(jnp.bfloat16)

    results = lax.map(one_item, jnp.arange(blocks * kv_count, dtype=jnp.int32))
    results = results.reshape(blocks, kv_count, block, group_size, head_width).transpose(
        0, 2, 1, 3, 4
    )
    return results.reshape(count_q, kv_count * group_size * head_width)


def rms_scale(values, gain_vec):
    floats = values.astype(jnp.float32)
    return (
        floats * lax.rsqrt(jnp.mean(floats * floats, axis=-1, keepdims=True) + EPSILON) * gain_vec
    )


def expert_ffn(arrived, gate_weight, up_weight, down_weight):
    gated = jnp.einsum("nesd,edf->nesf", arrived, gate_weight, preferred_element_type=jnp.float32)
    lifted = jnp.einsum("nesd,edf->nesf", arrived, up_weight, preferred_element_type=jnp.float32)
    hidden = (jax.nn.silu(gated) * lifted).astype(jnp.bfloat16)
    return jnp.einsum(
        "nesf,efd->nesd", hidden, down_weight, preferred_element_type=jnp.float32
    ).astype(jnp.bfloat16)


def local_any(
    residual_in,
    query_proj,
    key_proj,
    value_proj,
    query_gain,
    key_gain,
    out_weight,
    post_gain,
    pre_gain,
    route_ids,
    group_weight,
    first_share,
    gate_weight,
    up_weight,
    down_weight,
):
    sp_count = lax.axis_size("sp")
    dp_count = lax.axis_size("dp")
    tokens = query_proj.shape[1]
    group_size = HEADS // KV_HEADS
    key_all, value_all = (
        lax.all_gather(key_proj, "sp", axis=1, tiled=True),
        lax.all_gather(value_proj, "sp", axis=1, tiled=True),
    )
    length = key_all.shape[1]
    key_positions = jnp.arange(length, dtype=jnp.int32)
    query_positions = lax.axis_index("sp") * tokens + jnp.arange(tokens, dtype=jnp.int32)
    query_turned = rotate_heads(
        query_proj.reshape(tokens, HEADS, HEAD_DIM), query_gain, query_positions
    )
    key_turned = rotate_heads(key_all.reshape(length, KV_HEADS, HEAD_DIM), key_gain, key_positions)
    attended = attend_blocks(
        query_turned.reshape(tokens, KV_HEADS, group_size, HEAD_DIM),
        key_turned,
        value_all.reshape(length, KV_HEADS, HEAD_DIM),
    )
    mixed = jnp.dot(attended, out_weight, preferred_element_type=jnp.float32).astype(jnp.bfloat16)
    stream = (residual_in[0].astype(jnp.float32) + rms_scale(mixed, post_gain)).astype(jnp.bfloat16)
    normed = rms_scale(stream, pre_gain).astype(jnp.bfloat16)
    model_width = normed.shape[1]
    local_experts = gate_weight.shape[0]
    expert_count = local_experts * sp_count * dp_count
    capacity = 4 * tokens // expert_count
    chosen = route_ids.reshape(2 * tokens)
    onehot = (chosen[:, None] == jnp.arange(expert_count, dtype=jnp.int32)[None, :]).astype(
        jnp.int32
    )
    earlier = jnp.cumsum(onehot, axis=0) - onehot
    slot_rank = jnp.sum(earlier * onehot, axis=1)
    slot_index = chosen * capacity + slot_rank
    source_row = (
        jnp.full((expert_count * capacity,), tokens, jnp.int32)
        .at[slot_index]
        .set(jnp.arange(2 * tokens, dtype=jnp.int32) // 2)
    )
    padded = jnp.concatenate([normed, jnp.zeros((1, model_width), jnp.bfloat16)], axis=0)
    outgoing = padded[source_row]
    shaped = outgoing.reshape(sp_count * dp_count, local_experts, capacity, model_width)
    answered = expert_ffn(
        lax.all_to_all(shaped, ("sp", "dp"), split_axis=0, concat_axis=0, tiled=True),
        gate_weight,
        up_weight,
        down_weight,
    )
    returned = lax.all_to_all(answered, ("sp", "dp"), split_axis=0, concat_axis=0, tiled=True)
    results = (
        returned.reshape(expert_count * capacity, model_width)[slot_index]
        .astype(jnp.float32)
        .reshape(tokens, 2, model_width)
    )
    share = first_share[0]
    weight_pair = group_weight[0][:, None] * jnp.stack([share, 1.0 - share], axis=1)
    combined = jnp.sum(weight_pair[:, :, None] * results, axis=1)
    return (
        (stream.astype(jnp.float32) + combined).astype(jnp.bfloat16).reshape(1, tokens, model_width)
    )


def solution_any(mesh):
    placed = (
        P("dp", "sp", None),
        P("dp", "sp", None),
        P("dp", "sp", None),
        P("dp", "sp", None),
        P(),
        P(),
        P(),
        P(),
        P(),
        P("dp", "sp", None),
        P("dp", "sp"),
        P("dp", "sp"),
        P(("sp", "dp"), None, None),
        P(("sp", "dp"), None, None),
        P(("sp", "dp"), None, None),
    )
    return jax.shard_map(
        local_any, mesh=mesh, in_specs=placed, out_specs=P("dp", "sp", None), check_vma=False
    )


def turn(raw, cos, sin, exchange, ones):
    floats = raw.astype(jnp.float32)
    squares = floats * floats
    coarse = squares.astype(jnp.bfloat16)
    fine = (squares - coarse.astype(jnp.float32)).astype(jnp.bfloat16)
    total = jnp.dot(
        jnp.concatenate([coarse, fine], axis=1), ones, preferred_element_type=jnp.float32
    )
    turned = jnp.dot(raw, exchange, preferred_element_type=jnp.float32)
    scale = lax.rsqrt(total * (1.0 / raw.shape[-1]) + EPSILON)
    return ((floats * cos + turned * sin) * scale).astype(jnp.bfloat16)


def attend_kernel(blocks, weights, block_ids, query, row_table, col_table, *rest):
    kv = rest[:blocks]
    sources = rest[blocks : blocks + weights]
    attended = rest[blocks + weights]
    loaded = rest[blocks + weights + 1 : blocks + 2 * weights + 1]
    keys, values, turned, semaphores = rest[blocks + 2 * weights + 1 :]
    copies = [
        pltpu.make_async_copy(source, target, semaphores.at[index])
        for index, (source, target) in enumerate(zip(sources, loaded))
    ]
    for copy in copies:
        copy.start()
    tokens, _ = query.shape
    lines = tokens // GRID_W
    key_width = KV_HEADS * HEAD_DIM
    group = HEADS // KV_HEADS
    quarter = HEAD_DIM // 4
    source = lax.broadcasted_iota(jnp.int32, (HEAD_DIM, HEAD_DIM), 0)
    target = lax.broadcasted_iota(jnp.int32, (HEAD_DIM, HEAD_DIM), 1)
    partner = jnp.where((target // quarter) % 2 == 0, target + quarter, target - quarter)
    exchange = (source == partner).astype(jnp.bfloat16)
    ones = jnp.ones((2 * HEAD_DIM, HEAD_DIM), jnp.bfloat16)

    def table(block, which):
        cos, sin = [], []
        for line in range(lines):
            row = pl.ds(block_ids[block] * lines + line, 1)
            cos.append(row_table[which, 0, row, :] + col_table[which, 0])
            sin.append(row_table[which, 1, row, :] + col_table[which, 1])
        return jnp.concatenate(cos, axis=0), jnp.concatenate(sin, axis=0)

    for block in range(blocks):
        here = slice(block * tokens, (block + 1) * tokens)
        values[here, :] = kv[block][:, key_width:]
        cos, sin = table(block, 1)
        for head in range(KV_HEADS):
            columns = slice(head * HEAD_DIM, (head + 1) * HEAD_DIM)
            keys[here, columns] = turn(kv[block][:, columns], cos, sin, exchange, ones)

    cos, sin = table(blocks, 0)
    for head in range(HEADS):
        columns = slice(head * HEAD_DIM, (head + 1) * HEAD_DIM)
        turned[:, columns] = turn(query[:, columns], cos, sin, exchange, ones)

    factor = HEAD_DIM**-0.5 * 1.4426950408889634

    @pl.loop(0, KV_HEADS)
    def _(head):
        columns = pl.ds(pl.multiple_of(head * HEAD_DIM, HEAD_DIM), HEAD_DIM)
        for part in range(group):
            wide = pl.ds(pl.multiple_of((head * group + part) * HEAD_DIM, HEAD_DIM), HEAD_DIM)
            scores = lax.dot_general(
                turned[:, wide],
                keys[:, columns],
                (((1,), (1,)), ((), ())),
                preferred_element_type=jnp.float32,
            )
            top = jnp.max(scores, axis=-1, keepdims=True)
            shifted = jnp.exp2((scores - top) * factor)
            total = jnp.sum(shifted, axis=-1, keepdims=True)
            result = jnp.dot(
                shifted.astype(jnp.bfloat16),
                values[:, columns],
                preferred_element_type=jnp.float32,
            )
            attended[:, wide] = (result * (1.0 / total)).astype(jnp.bfloat16)

    for copy in copies:
        copy.wait()


def out_kernel(chunks, residual, meta, gains, attended, weight, *rest):
    stream_out = rest[0]
    row_outs = rest[1 : 1 + chunks]
    mixed, payload = rest[1 + chunks :]
    tokens, width = residual.shape
    step = 4 * HEAD_DIM

    @pl.loop(0, width // step)
    def _(index):
        columns = pl.ds(pl.multiple_of(index * step, step), step)
        mixed[:, columns] = jnp.dot(
            attended[...], weight[:, columns], preferred_element_type=jnp.float32
        ).astype(jnp.bfloat16)

    raw = mixed[...].astype(jnp.float32)
    scaled = (
        raw * lax.rsqrt(jnp.mean(raw * raw, axis=-1, keepdims=True) + EPSILON) * gains[0:1]
    )
    stream = (residual[...].astype(jnp.float32) + scaled).astype(jnp.bfloat16)
    stream_out[...] = stream
    floats = stream.astype(jnp.float32)
    payload[:, :width] = (
        floats
        * lax.rsqrt(jnp.mean(floats * floats, axis=-1, keepdims=True) + EPSILON)
        * gains[1:2]
    ).astype(jnp.bfloat16)
    payload[:, width:] = meta[...]
    slot = meta[:, LANES - 1 :].astype(jnp.float32)
    place = lax.broadcasted_iota(jnp.int32, (tokens, tokens), 1).astype(jnp.float32)
    choose = (slot == place).astype(jnp.bfloat16)
    ordered = lax.dot_general(
        choose, payload[...], (((0,), (0,)), ((), ())), preferred_element_type=jnp.float32
    ).astype(jnp.bfloat16)
    rows = tokens // chunks
    for chunk in range(chunks):
        row_outs[chunk][...] = ordered[chunk * rows : (chunk + 1) * rows]


def expert_kernel(count, which, gate, up, down, *rest):
    inputs = rest[:count]
    outputs = rest[count:]
    width = gate.shape[0]
    block = jnp.concatenate([ref[:, :width] for ref in inputs], axis=0)
    meta = jnp.concatenate([ref[:, width:] for ref in inputs], axis=0).astype(jnp.float32)
    lane = lax.broadcasted_iota(jnp.int32, meta.shape, 1)
    mine = (lane == which[0]) | (lane == which[0] + LANES // 2)
    share = jnp.sum(jnp.where(mine, meta, 0.0), axis=-1, keepdims=True)
    gated = jnp.dot(block, gate[...], preferred_element_type=jnp.float32)
    lifted = jnp.dot(block, up[...], preferred_element_type=jnp.float32)
    hidden = (gated / (1.0 + jnp.exp(-gated)) * lifted).astype(jnp.bfloat16)
    produced = jnp.dot(hidden, down[...], preferred_element_type=jnp.float32).astype(jnp.bfloat16)
    weighted = (produced.astype(jnp.float32) * share).astype(jnp.bfloat16)
    base = 0
    for ref in outputs:
        ref[...] = weighted[base : base + ref.shape[0]]
        base += ref.shape[0]


def last_kernel(chunks, stream, meta, *rest):
    returned = rest[:chunks]
    out = rest[chunks]
    tokens = stream.shape[0]
    slot = meta[:, LANES - 1 :].astype(jnp.float32)
    place = lax.broadcasted_iota(jnp.int32, (tokens, tokens), 1).astype(jnp.float32)
    choose = (slot == place).astype(jnp.bfloat16)
    block = jnp.concatenate([ref[...] for ref in returned], axis=0)
    added = jnp.dot(choose, block, preferred_element_type=jnp.float32)
    out[...] = (stream[...].astype(jnp.float32) + added).astype(jnp.bfloat16)


VMEM = pl.BlockSpec(memory_space=pltpu.VMEM)
HBM = pl.BlockSpec(memory_space=pltpu.HBM)
SMEM = pl.BlockSpec(memory_space=pltpu.SMEM)


def shape_of(*dims):
    return jax.ShapeDtypeStruct(dims, jnp.bfloat16)


def local_plane(
    residual_in,
    query_proj,
    key_proj,
    value_proj,
    query_gain,
    key_gain,
    out_weight,
    post_gain,
    pre_gain,
    route_ids,
    group_weight,
    first_share,
    gate_weight,
    up_weight,
    down_weight,
):
    planes = lax.axis_size("z")
    xs, ys, cores = lax.axis_size("x"), lax.axis_size("y"), lax.axis_size("c")
    z, x, y, c = (lax.axis_index(name) for name in ("z", "x", "y", "c"))
    tokens, width = query_proj.shape[1:]
    rows = tokens // planes
    members = xs * ys * cores
    blocks = planes * cores

    def carry(value, jump):
        flat = lambda a, b, d: (a * xs + b) * cores + d
        route = [
            (flat(a, b, d), flat((a + jump) % planes, d, b))
            for a, b, d in itertools.product(range(planes), range(xs), range(cores))
        ]
        return lax.ppermute(value, ("z", "x", "c"), route)

    def shift(value, jump):
        return lax.ppermute(value, "z", [(a, (a + jump) % planes) for a in range(planes)])

    def swap(value, axis):
        return lax.ppermute(value, axis, [(0, 1), (1, 0)])

    kv = jnp.concatenate([key_proj[0], value_proj[0]], axis=1)
    kv_here = [None] * planes
    for jump in reversed(range(planes)):
        kv_here[jump] = carry(kv, jump)
    query = carry(query_proj[0], 0)
    residual = carry(residual_in[0], 0)
    kv_there = [None] * planes
    for jump in reversed(range(planes)):
        kv_there[jump] = swap(kv_here[jump], "c")

    ids = route_ids[0]
    group = ids[:, 0] // members
    jump_of = (group - z) % planes
    onehot = (group[:, None] == jnp.arange(planes, dtype=jnp.int32)).astype(jnp.float32)
    earlier = jnp.tril(jnp.ones((tokens, tokens), jnp.float32), -1)
    rank = jnp.sum(jnp.dot(earlier, onehot) * onehot, axis=1)
    slot = jump_of.astype(jnp.float32) * rows + rank
    share = first_share[0]
    pair = group_weight[0][:, None] * jnp.stack([share, 1.0 - share], axis=1)
    half = LANES // 2
    lane = jnp.arange(LANES, dtype=jnp.int32)
    spread = jnp.where((ids[:, :1] % members) == lane % half, pair[:, :1], 0.0) + jnp.where(
        (ids[:, 1:] % members) == lane % half, pair[:, 1:], 0.0
    )
    coarse = lax.reduce_precision(spread, 8, 7)
    meta = jnp.where(lane < half, coarse, spread - coarse)
    meta = jnp.where(lane == LANES - 1, slot[:, None], meta).astype(jnp.bfloat16)
    meta_here = carry(meta, 0)

    order = [(z - jump) % planes for jump in range(planes)]
    block_ids = jnp.stack(
        [a * cores + c for a in order] + [a * cores + (1 - c) for a in order] + [z * cores + c]
    ).astype(jnp.int32)
    quarter = HEAD_DIM // 4
    inverse = 10000.0 ** (-jnp.arange(quarter, dtype=jnp.float32) / quarter)
    lines = blocks * tokens // GRID_W

    def turns(count, columns):
        angles = jnp.arange(count, dtype=jnp.float32)[:, None] * inverse
        zeros = [jnp.zeros((count, 2 * quarter), jnp.float32)]
        cos = [jnp.cos(angles)] * 2
        sin = [-jnp.sin(angles), jnp.sin(angles)]
        pad = lambda pieces: jnp.concatenate(
            zeros + pieces if columns else pieces + zeros, axis=1
        )
        made = []
        for gain in (query_gain, key_gain):
            crossed = gain.reshape(2, 2, quarter)[:, ::-1].reshape(-1)
            made.append(jnp.stack([pad(cos) * gain, pad(sin) * crossed]))
        return jnp.stack(made)

    payload = width + LANES
    key_width = KV_HEADS * HEAD_DIM
    length = blocks * tokens
    weights = (out_weight,)
    attended, mixing = pl.pallas_call(
        functools.partial(attend_kernel, blocks, len(weights)),
        out_shape=[shape_of(tokens, width)] + [shape_of(*item.shape) for item in weights],
        in_specs=[SMEM] + [VMEM] * (3 + blocks) + [HBM] * len(weights),
        out_specs=[VMEM] * (1 + len(weights)),
        scratch_shapes=[
            pltpu.VMEM((length, key_width), jnp.bfloat16),
            pltpu.VMEM((length, key_width), jnp.bfloat16),
            pltpu.VMEM((tokens, width), jnp.bfloat16),
            pltpu.SemaphoreType.DMA((len(weights),)),
        ],
        cost_estimate=pl.CostEstimate(
            flops=4 * tokens * width * length,
            bytes_accessed=2 * length * 2 * key_width,
            transcendentals=tokens * HEADS * length,
        ),
        compiler_params=pltpu.CompilerParams(vmem_limit_bytes=40 << 20),
        name="attend",
    )(
        block_ids,
        query,
        turns(lines, False),
        turns(GRID_W, True),
        *kv_here,
        *kv_there,
        *weights,
    )
    made = pl.pallas_call(
        functools.partial(out_kernel, planes),
        out_shape=[shape_of(tokens, width)] + [shape_of(rows, payload)] * planes,
        in_specs=[VMEM] * 5,
        out_specs=[VMEM] * (1 + planes),
        scratch_shapes=[
            pltpu.VMEM((tokens, width), jnp.bfloat16),
            pltpu.VMEM((tokens, payload), jnp.bfloat16),
        ],
        cost_estimate=pl.CostEstimate(
            flops=2 * tokens * width * width,
            bytes_accessed=2 * width * width,
            transcendentals=0,
        ),
        compiler_params=pltpu.CompilerParams(vmem_limit_bytes=24 << 20),
        name="project",
    )(residual, meta_here, jnp.stack([post_gain, pre_gain]), attended, mixing)
    stream_here, sorted_rows = made[0], made[1:]
    arrived = []
    for jump, value in enumerate(sorted_rows):
        arrived.append(carry(value, jump))
    stream = carry(stream_here, 0)

    middle = tokens // 2
    per_half = planes // 2
    top = jnp.concatenate(arrived[:per_half], axis=0)
    bottom = jnp.concatenate(arrived[per_half:], axis=0)

    x_top, y_top = swap(top, "x"), swap(top, "y")
    y_bottom, x_bottom = swap(bottom, "y"), swap(bottom, "x")
    far_top = swap(y_top, "x")
    far_bottom = swap(x_bottom, "y")
    which = ((x * ys + y) * cores + c).reshape(1).astype(jnp.int32)

    def experts(first, second):
        block = jnp.concatenate([first, second], axis=0)
        inputs = [block, swap(block, "c")]
        count = len(inputs)
        total = 2 * tokens
        kept, sent = pl.pallas_call(
            functools.partial(expert_kernel, count),
            out_shape=[shape_of(tokens, width)] * cores,
            in_specs=[SMEM] + [VMEM] * (3 + count),
            out_specs=[VMEM] * cores,
            cost_estimate=pl.CostEstimate(
                flops=6 * total * width * gate_weight.shape[2],
                bytes_accessed=6 * width * gate_weight.shape[2],
                transcendentals=total * gate_weight.shape[2],
            ),
            compiler_params=pltpu.CompilerParams(vmem_limit_bytes=20 << 20),
            name="experts",
        )(which, gate_weight[0], up_weight[0], down_weight[0], *inputs)
        other = swap(sent, "c")
        halves = kept[:middle] + other[:middle], kept[middle:] + other[middle:]
        return lax.optimization_barrier(halves)

    sum_own = experts(top, bottom)
    sum_x = experts(x_top, x_bottom)
    sum_y = experts(y_top, y_bottom)
    sum_far = experts(far_top, far_bottom)
    back_x = swap(sum_x[0], "x")
    back_y = swap(sum_y[1], "y")
    low_y = sum_y[0] + swap(sum_far[0], "x")
    high_x = sum_x[1] + swap(sum_far[1], "y")
    summed = [sum_own[0] + back_x + swap(low_y, "y"), sum_own[1] + back_y + swap(high_x, "x")]
    returned = []
    for jump in range(planes):
        half, start = summed[jump // per_half], (jump % per_half) * rows
        part = half[start : start + rows]
        returned.append(shift(part, -jump) if jump else part)
    result = pl.pallas_call(
        functools.partial(last_kernel, planes),
        out_shape=shape_of(tokens, width),
        in_specs=[VMEM] * (2 + planes),
        out_specs=VMEM,
        cost_estimate=pl.CostEstimate(
            flops=2 * tokens * tokens * width, bytes_accessed=6 * tokens * width, transcendentals=0
        ),
        compiler_params=pltpu.CompilerParams(vmem_limit_bytes=8 << 20),
        name="last",
    )(stream, meta, *returned)
    return result[None]


def solution(mesh):
    sp_count, dp_count = mesh.shape["sp"], mesh.shape["dp"]
    xs, ys = sp_count // GROUPS, dp_count // CORES
    if (xs, ys) != (2, 2) or xs != CORES:
        return solution_any(mesh)
    fine = Mesh(mesh.devices.reshape(GROUPS, xs, ys, CORES), ("z", "x", "y", "c"))
    tokens = P(("y", "c"), ("z", "x"), None)
    scalars = P(("y", "c"), ("z", "x"))
    experts = P(("z", "x", "y", "c"), None, None)
    placed = (tokens,) * 4 + (P(),) * 5 + (tokens, scalars, scalars) + (experts,) * 3
    return jax.shard_map(
        local_plane, mesh=fine, in_specs=placed, out_specs=tokens, check_vma=False
    )
```
